32 devices in a mesh: grp: 2 (over y), sp: 4 (over z), tp: 4 (over x, core).
Axes of the slice: x: 2, y: 2, z: 4, core: 2. Of those that a mesh axis runs over, the one named last changes fastest.
Arguments:
- tokens: bfloat16 [2048, 8, 2048], P('sp', 'grp'), parts along dimension 1, may hold values from -48 to 48
- query_weight: bfloat16 [2048, 1024], P(None, 'tp'), may hold values from -2 to 2
- key_weight: bfloat16 [2048, 1024], P(None, 'tp'), may hold values from -2 to 2
- value_weight: bfloat16 [2048, 1024], P(None, 'tp'), may hold values from -3 to 3
- mix_gain: float32 [1024], P('tp'), may hold values from 0.1 to 1.9
- out_weight: bfloat16 [1024, 2048], P('tp'), may hold values from -0.1875 to 0.1875
Outputs:
- mixed: bfloat16 [2048, 8, 2048], P(('sp', 'tp'), 'grp'), parts along dimension 1
The draws below stay inside these ranges and needn't reach their ends.
There are 2 independent parts, one for each index of `grp`. The reference program is written for one: setup_inputs(seed, part) draws one part's arguments, and reference() takes and returns one part's arrays. A program takes and returns all parts, laid end to end along the dimension named above; an argument that names none is the same for every part. Nothing has to cross between parts.
All inputs are finite; a program needn't handle non-finite values.
Results may differ from the reference program's by a relative error of at most 0.02.
Values may be sent and summed in bfloat16 or wider, within the bound.
A program may use at most 128 MiB of HBM per device.

```python
import jax
import jax.numpy as jnp
from jax import lax

D = 2048
HEADS = 16
HEAD_DIM = 64
A_W = 1024
BATCH = 4
SEQ = 2048
N_TP = 4


def draw_tokens(key, part):
    normal_part = jax.random.normal(jax.random.fold_in(key, 1), (SEQ, BATCH, D), jnp.float32)
    result = jnp.clip(normal_part, -6.0, 6.0)
    return result.astype(jnp.bfloat16)


def projection_pair(key):
    leading = jnp.clip(jax.random.normal(jax.random.fold_in(key, 11), (D, A_W), jnp.float32), -6.0, 6.0)
    partner = jnp.clip(jax.random.normal(jax.random.fold_in(key, 12), (D, A_W), jnp.float32), -6.0, 6.0)
    return (leading * D ** (-0.5), partner * D ** (-0.5))


def draw_query_weight(key, part):
    leading, partner = projection_pair(key)
    return leading.astype(jnp.bfloat16)


def draw_key_weight(key, part):
    leading, partner = projection_pair(key)
    blended = partner
    return blended.astype(jnp.bfloat16)


def draw_value_weight(key, part):
    normal_part = jnp.clip(jax.random.normal(jax.random.fold_in(key, 21), (D, A_W), jnp.float32), -6.0, 6.0)
    factors = jnp.exp(jax.random.uniform(jax.random.fold_in(key, 22), (HEADS,), jnp.float32, -1.1, 1.1))
    scaled = normal_part * D ** (-0.5) * jnp.repeat(factors, HEAD_DIM)[None, :]
    return scaled.astype(jnp.bfloat16)


def levels(rng, shape, split, smallest, high):
    loudness, own = 1.0, jax.random.fold_in(rng, 6)
    for dim, shards_of in split:
        draws = jnp.exp(jax.random.uniform(jax.random.fold_in(own, dim), (shards_of,), jnp.float32, smallest / len(split), high / len(split)))
        loudness = loudness * jnp.repeat(draws, shape[dim] // shards_of).reshape([-1 if axis == dim else 1 for axis in range(len(shape))])
    return loudness


def bell_draw(rng, extent, spread, most, shards=(), held_as=jnp.bfloat16):
    loudness = levels(rng, extent, shards, -0.22, 0.18) if shards else 1.0
    entries = jax.random.normal(rng, extent, jnp.float32) * spread * loudness
    return jnp.minimum(jnp.maximum(entries, -most), most).astype(held_as)


def setup_inputs(seed: int = 0, part: int = 0) -> dict:
    streams_of = jax.random.split(jax.random.key(seed), 7)
    part_keys = jax.random.split(jax.random.fold_in(streams_of[6], part), 7)
    return {
        "tokens": draw_tokens(jax.random.fold_in(jax.random.fold_in(streams_of[6], part), 71), part),
        "query_weight": draw_query_weight(jax.random.fold_in(streams_of[6], 71), part),
        "key_weight": draw_key_weight(jax.random.fold_in(streams_of[6], 71), part),
        "value_weight": draw_value_weight(jax.random.fold_in(streams_of[6], 71), part),
        "mix_gain": jnp.clip(1.0 + 0.18 * jax.random.normal(streams_of[4], (A_W,), jnp.float32), 0.1, 1.9),
        "out_weight": bell_draw(streams_of[5], (A_W, D), A_W ** -0.5, 0.1875, ((0, 4),)),
    }


PATTERNS = ((128, 1), (512, 4), (2048, 16))
REACH = 128
EPSILON = 1e-06
NEGATIVE = -1e+30

def band_attend(queries, key_rows, value_rows, live_mask):
    lead_shape = queries.shape[:3]
    query_len = queries.shape[3]
    head_size = queries.shape[4]
    block_len = min(REACH, query_len)
    block_count = query_len // block_len
    query_blocks = queries.reshape(lead_shape + (block_count, block_len, head_size))
    if block_count == 1:
        key_ctx = key_rows.reshape(lead_shape + (1, query_len + REACH, head_size))
        value_ctx = value_rows.reshape(lead_shape + (1, query_len + REACH, head_size))
        live_ctx = live_mask.reshape((live_mask.shape[0], 1, query_len + REACH))
    else:
        key_blocks = key_rows.reshape(lead_shape + (block_count + 1, REACH, head_size))
        value_blocks = value_rows.reshape(lead_shape + (block_count + 1, REACH, head_size))
        key_ctx = jnp.concatenate([key_blocks[:, :, :, :-1], key_blocks[:, :, :, 1:]], axis=4)
        value_ctx = jnp.concatenate([value_blocks[:, :, :, :-1], value_blocks[:, :, :, 1:]], axis=4)
        live_blocks = live_mask.reshape((live_mask.shape[0], block_count + 1, REACH))
        live_ctx = jnp.concatenate([live_blocks[:, :-1], live_blocks[:, 1:]], axis=2)
    ctx_width = block_len + REACH
    offset = jnp.arange(ctx_width)[None, :] - jnp.arange(block_len)[:, None]
    in_band = (offset >= 0) & (offset <= REACH)
    valid = in_band[None, None] & live_ctx[:, :, None, :]
    scores = jnp.einsum('gbhnqe,gbhnke->gbhnqk', query_blocks.astype(jnp.float32), key_ctx.astype(jnp.float32)) * head_size ** (-0.5)
    scores = jnp.where(valid[:, None, None], scores, NEGATIVE)
    highest = lax.optimization_barrier(jnp.max(scores, axis=-1, keepdims=True))
    raised = jnp.exp(scores - highest)
    totals = lax.optimization_barrier(jnp.sum(raised, axis=-1, keepdims=True))
    probs = (raised / totals).astype(jnp.bfloat16)
    result = jnp.einsum('gbhnqk,gbhnke->gbhnqe', probs.astype(jnp.float32), value_ctx.astype(jnp.float32)).astype(jnp.bfloat16)
    log_norm = (highest + jnp.log(totals))[..., 0]
    return (result.reshape(lead_shape + (query_len, head_size)), log_norm.reshape(lead_shape + (query_len,)))

def dilated_pattern(queries, context, base, window, stride):
    seq_rows, batch_size, channels = queries.shape
    heads_dev = channels // HEAD_DIM
    query_len = seq_rows // stride
    key_len = query_len + REACH
    query_class = queries.reshape(query_len, stride, batch_size, heads_dev, HEAD_DIM).transpose(1, 2, 3, 0, 4)
    keyval_class = context.reshape(key_len, stride, batch_size, 2 * heads_dev, HEAD_DIM).transpose(1, 2, 3, 0, 4)
    position = jnp.arange(key_len)[None, :] * stride + jnp.arange(stride)[:, None] + base
    result, log_norm = band_attend(query_class, keyval_class[:, :, :heads_dev], keyval_class[:, :, heads_dev:], position >= 0)
    result = result.transpose(3, 0, 1, 2, 4).reshape(seq_rows, batch_size, channels)
    log_norm = log_norm.transpose(3, 0, 1, 2).reshape(seq_rows, batch_size, heads_dev)
    return (result, log_norm)

def reference(tokens, query_weight, key_weight, value_weight, mix_gain, out_weight):
    seq_len, batch_size, width = tokens.shape
    flat = tokens.reshape(seq_len * batch_size, width)

    def project(weight):
        product = jnp.dot(flat, weight, preferred_element_type=jnp.float32).astype(jnp.bfloat16)
        return product.reshape(seq_len, batch_size, weight.shape[1])
    queries = project(query_weight)
    key_values = jnp.concatenate([project(key_weight), project(value_weight)], axis=-1)
    channels = queries.shape[2]
    heads_all = channels // HEAD_DIM

    def one_sequence(pair):
        query_seq, keyval_seq = pair
        query_seq = query_seq[:, None]
        keyval_seq = keyval_seq[:, None]
        results = []
        norms = []
        for window, stride in PATTERNS:
            context = jnp.pad(keyval_seq, ((window, 0), (0, 0), (0, 0)))
            result, log_norm = dilated_pattern(query_seq, context, -window, window, stride)
            results.append(result)
            norms.append(log_norm)
        weights = jax.nn.softmax(jnp.stack(norms, axis=0), axis=0)
        combined = jnp.zeros((seq_len, 1, heads_all, HEAD_DIM), jnp.float32)
        for index in range(len(PATTERNS)):
            combined = combined + weights[index][..., None] * results[index].astype(jnp.float32).reshape(seq_len, 1, heads_all, HEAD_DIM)
        return combined.reshape(seq_len, channels)
    combined = lax.map(one_sequence, (queries.transpose(1, 0, 2), key_values.transpose(1, 0, 2)))
    combined = combined.transpose(1, 0, 2)
    mean_square = lax.optimization_barrier(jnp.sum(combined * combined, axis=-1, keepdims=True)) / channels
    normed = (combined * lax.rsqrt(mean_square + EPSILON) * mix_gain.astype(jnp.float32)).astype(jnp.bfloat16)
    group = channels // N_TP
    total = jnp.zeros((seq_len * batch_size, out_weight.shape[1]), jnp.float32)
    for member in range(N_TP):
        block = normed[..., member * group:(member + 1) * group].reshape(seq_len * batch_size, group)
        partial_out = jnp.dot(block, out_weight[member * group:(member + 1) * group], preferred_element_type=jnp.float32).astype(jnp.bfloat16)
        total = total + partial_out.astype(jnp.float32)
    return total.reshape(seq_len, batch_size, out_weight.shape[1]).astype(jnp.bfloat16)
```

```python
import functools

import jax
import jax.numpy as jnp
from jax import lax
from jax.experimental import pallas as pl
from jax.experimental.pallas import tpu as pltpu
from jax.sharding import PartitionSpec as P

HEAD_DIM = 64
PATTERNS = ((128, 1), (512, 4), (2048, 16))
REACH = 128
CLASSES = 16
EPSILON = 1e-06
NEGATIVE = -1e30
GROUPS = 2


def attend_kernel(q_ref, k_ref, v_ref, o_ref, out_sc, top_sc, sum_sc, near_bias, mid_bias, far_bias):
    chunks, _, per_class, width = q_ref.shape
    heads = width // HEAD_DIM
    tile = 16
    near_rows = CLASSES * tile
    mid_rows = 4 * per_class
    span = REACH // per_class
    far_tiles = chunks // span

    def bias_of(diff, window, live):
        return jnp.where((diff >= 0) & (diff <= window) & live, 0.0, NEGATIVE).astype(jnp.float32)

    row = lax.broadcasted_iota(jnp.int32, near_bias.shape[1:], 0)
    col = lax.broadcasted_iota(jnp.int32, near_bias.shape[1:], 1)
    diff = (row % tile - col % tile) * 16 + row // tile - (col % near_rows) // tile
    diff = diff + jnp.where(col < near_rows, near_rows, 0)
    near_bias[0] = bias_of(diff, PATTERNS[0][0], col >= near_rows)
    near_bias[1] = bias_of(diff, PATTERNS[0][0], col >= 0)
    row = lax.broadcasted_iota(jnp.int32, mid_bias.shape[1:], 0)
    col = lax.broadcasted_iota(jnp.int32, mid_bias.shape[1:], 1)
    diff = (row % per_class - col % per_class) * 16
    diff = diff + 4 * (row // per_class - (col % mid_rows) // per_class)
    diff = diff + jnp.where(col < mid_rows, CLASSES * per_class, 0)
    mid_bias[0] = bias_of(diff, PATTERNS[1][0], col >= mid_rows)
    mid_bias[1] = bias_of(diff, PATTERNS[1][0], col >= 0)
    row = lax.broadcasted_iota(jnp.int32, far_bias.shape, 0)
    col = lax.broadcasted_iota(jnp.int32, far_bias.shape, 1)
    far_bias[...] = bias_of(row + REACH - col, REACH, col >= 0)

    lane = lax.broadcasted_iota(jnp.int32, (1, width), 1) // HEAD_DIM
    picks = [jnp.where(lane == h, HEAD_DIM ** -0.5, 0.0).astype(jnp.bfloat16) for h in range(heads)]

    def attend(queries, keys, values, bias):
        outs, tops, sums = [], [], []
        for h in range(heads):
            scores = lax.dot_general(
                queries * picks[h], keys, (((1,), (1,)), ((), ())), preferred_element_type=jnp.float32
            ) + bias
            top = jnp.max(scores, axis=1, keepdims=True)
            raised = jnp.exp(scores - top)
            total = jnp.sum(raised, axis=1, keepdims=True)
            outs.append(jnp.dot(raised.astype(jnp.bfloat16), values, preferred_element_type=jnp.float32))
            tops.append(jnp.broadcast_to(top, outs[-1].shape))
            sums.append(jnp.broadcast_to(total, outs[-1].shape))

        def join(parts):
            whole = parts[0]
            for h in range(1, heads):
                whole = jnp.where(lane == h, parts[h], whole)
            return whole

        return join(outs), join(tops), join(sums)

    def merge_rows(ref, *index):
        block = ref[index]
        return block.reshape(-1, width)

    @pl.loop(0, chunks)
    def near_and_mid(z):
        before = jnp.maximum(z - 1, 0)
        first = jnp.minimum(z, 1)
        for u in range(per_class // tile):
            rows = slice(u * tile, (u + 1) * tile)
            back, back_rows, kind = (before, slice(per_class - tile, per_class), first)
            if u > 0:
                back, back_rows, kind = (z, slice((u - 1) * tile, u * tile), 1)
            queries = q_ref[z, :, rows, :].reshape(near_rows, width)
            keys, values = (
                jnp.concatenate(
                    [
                        ref[back, :, back_rows, :].reshape(near_rows, width),
                        ref[z, :, rows, :].reshape(near_rows, width),
                    ],
                    axis=0,
                )
                for ref in (k_ref, v_ref)
            )
            for ref, part in zip((out_sc, top_sc, sum_sc), attend(queries, keys, values, near_bias[kind])):
                ref[0, z, :, rows, :] = part.reshape(CLASSES, tile, width)
        for r in range(4):
            classes = range(r, CLASSES, 4)
            queries = jnp.concatenate([q_ref[z, c] for c in classes], axis=0)
            keys, values = (
                jnp.concatenate([ref[y, c] for y in (before, z) for c in classes], axis=0)
                for ref in (k_ref, v_ref)
            )
            for ref, part in zip((out_sc, top_sc, sum_sc), attend(queries, keys, values, mid_bias[first])):
                for m, c in enumerate(classes):
                    ref[1, z, c] = part[m * per_class : (m + 1) * per_class]

    @pl.loop(0, CLASSES // 4)
    def far(quad):
        for inner in range(4):
            c = quad * 4 + inner
            for n in range(far_tiles):
                here = slice(n * span, (n + 1) * span)
                reach = slice(max(n - 1, 0) * span, (n + 1) * span)
                queries = q_ref[here, c].reshape(REACH, width)
                keys, values = (ref[reach, c].reshape(-1, width) for ref in (k_ref, v_ref))
                bias = far_bias[...] if n > 0 else far_bias[:, REACH:]
                for ref, part in zip((out_sc, top_sc, sum_sc), attend(queries, keys, values, bias)):
                    ref[2, here, c] = part.reshape(span, per_class, width)

    @pl.loop(0, chunks)
    def mix(z):
        tops = [top_sc[p, z] for p in range(3)]
        highest = jnp.maximum(jnp.maximum(tops[0], tops[1]), tops[2])
        lifts = [jnp.exp(top - highest) for top in tops]
        total = sum(lift * sum_sc[p, z] for p, lift in enumerate(lifts))
        result = sum(lift * out_sc[p, z] for p, lift in enumerate(lifts))
        o_ref[z] = (result / total).astype(o_ref.dtype)


def attend_all(moved, width):
    chunks, batches, _, per_class, triple = moved.shape
    channels = triple // 3
    pairs = channels // width
    if width % 128 == 0:
        operands = (moved, moved, moved)
        starts = (0, pairs, 2 * pairs)
    else:
        operands = tuple(moved[..., i * channels : (i + 1) * channels] for i in range(3))
        starts = (0, 0, 0)
    block = (chunks, None, CLASSES, per_class, width)
    tokens = chunks * CLASSES * per_class
    return pl.pallas_call(
        attend_kernel,
        grid=(batches, pairs),
        in_specs=[
            pl.BlockSpec(block, functools.partial(lambda s, b, i: (0, b, 0, 0, s + i), start)) for start in starts
        ],
        out_specs=pl.BlockSpec(block, lambda b, i: (0, b, 0, 0, i)),
        out_shape=jax.ShapeDtypeStruct((chunks, batches, CLASSES, per_class, channels), jnp.bfloat16),
        scratch_shapes=[pltpu.VMEM((3, chunks, CLASSES, per_class, width), jnp.float32) for _ in range(3)]
        + [
            pltpu.VMEM((2, 256, 512), jnp.float32),
            pltpu.VMEM((2, 4 * per_class, 8 * per_class), jnp.float32),
            pltpu.VMEM((REACH, 2 * REACH), jnp.float32),
        ],
        cost_estimate=pl.CostEstimate(
            flops=tokens * batches * channels * 4 * 900,
            bytes_accessed=tokens * batches * channels * 8,
            transcendentals=tokens * batches * channels // HEAD_DIM * 900,
        ),
    )(*operands)


def body(tokens, query_weight, key_weight, value_weight, mix_gain, out_weight):
    seq_rows, batch_size, features = tokens.shape
    channels = query_weight.shape[1]
    sp_count = lax.axis_size("sp")
    tp_count = lax.axis_size("tp")
    tp_place = lax.axis_index("tp")
    per_class = seq_rows // CLASSES
    head_split = min(max(1, sp_count // batch_size), channels // HEAD_DIM)
    copies = max(1, sp_count // (batch_size * head_split))
    batches = max(1, batch_size // sp_count)
    groups = GROUPS if head_split == 1 else 1

    own = (out_weight.astype(jnp.float32) * mix_gain[:, None]).astype(jnp.bfloat16)
    gathered = [own]
    for step in range(1, tp_count):
        route = [(i, (i + step) % tp_count) for i in range(tp_count)]
        gathered.append(lax.ppermute(own, "tp", route))

    flat = tokens.reshape(per_class, CLASSES, batch_size, features).transpose(2, 1, 0, 3)
    flat = flat.reshape(batch_size * seq_rows, features)
    cut = channels // groups // head_split
    width = min(cut, 2 * HEAD_DIM)
    results = []
    for g in range(groups):
        columns = []
        for s in range(head_split):
            at = (g * head_split + s) * cut
            columns += [w[:, at : at + cut] for w in (query_weight, key_weight, value_weight)]
        product = jnp.dot(flat, jnp.concatenate(columns, axis=1), preferred_element_type=jnp.float32)
        product = product.astype(jnp.bfloat16).reshape(batch_size, seq_rows, head_split, 3 * cut)
        if head_split > 1:
            product = product.transpose(0, 2, 1, 3)
        product = product.reshape(sp_count // copies, batches * seq_rows, 3 * cut)
        if copies > 1:
            product = jnp.repeat(product, copies, axis=0)
        moved = lax.all_to_all(product, "sp", split_axis=0, concat_axis=0, tiled=True)
        moved = moved.reshape(sp_count, batches, CLASSES, per_class, 3 * cut)
        results.append(attend_all(moved, width))

    part = per_class // tp_count
    backs = []
    for result in results:
        back = result.reshape(sp_count, batches, CLASSES, tp_count, part, cut).transpose(0, 3, 1, 2, 4, 5)
        back = back.reshape(sp_count * tp_count, batches * CLASSES * part, cut)
        back = lax.all_to_all(back, ("sp", "tp"), split_axis=0, concat_axis=0, tiled=True)
        back = back.reshape(batch_size // batches, head_split, copies, tp_count, batches, CLASSES, part, cut)[:, :, 0]
        backs.append(back)
    combined = jnp.stack(backs, axis=0).transpose(3, 6, 5, 1, 4, 0, 2, 7)
    rows = part * CLASSES * batch_size
    combined = combined.reshape(tp_count, rows, channels)
    flipped = combined[::-1]
    turned = lax.dynamic_slice_in_dim(
        jnp.concatenate([flipped, flipped], axis=0), tp_count - 1 - tp_place, tp_count, axis=0
    )
    turned = turned.transpose(1, 0, 2).reshape(rows, tp_count * channels)
    wide = turned.astype(jnp.float32)
    row_scale = lax.rsqrt(jnp.mean(wide * wide, axis=-1, keepdims=True) + EPSILON)
    mixed = jnp.dot(turned, jnp.concatenate(gathered, axis=0), preferred_element_type=jnp.float32) * row_scale
    return mixed.astype(jnp.bfloat16).reshape(part * CLASSES, batch_size, out_weight.shape[1])


def solution(mesh):
    in_specs = (
        P("sp", "grp", None),
        P(None, "tp"),
        P(None, "tp"),
        P(None, "tp"),
        P("tp"),
        P("tp", None),
    )
    out_specs = P(("sp", "tp"), "grp", None)
    return jax.shard_map(body, mesh=mesh, in_specs=in_specs, out_specs=out_specs, check_vma=False)
```

```python
import functools

import jax
import jax.numpy as jnp
from jax import lax
from jax.experimental import pallas as pl
from jax.experimental.pallas import tpu as pltpu
from jax.sharding import PartitionSpec as P

HEAD_DIM = 64
PATTERNS = ((128, 1), (512, 4), (2048, 16))
REACH = 128
CLASSES = 16
LANES = 128
EPSILON = 1e-06
NEGATIVE = -1e30
GROUPS = 2


def attend_kernel(q_ref, k_ref, v_ref, o_ref, out_sc, top_sc, sum_sc, near_bias, mid_bias, far_bias):
    chunks, _, per_class, width = q_ref.shape
    heads = width // HEAD_DIM
    tile = 16
    near_rows = CLASSES * tile
    mid_rows = 4 * per_class
    span = REACH // per_class
    far_tiles = chunks // span

    def bias_of(diff, window, live):
        return jnp.where((diff >= 0) & (diff <= window) & live, 0.0, NEGATIVE).astype(jnp.float32)

    row = lax.broadcasted_iota(jnp.int32, near_bias.shape[1:], 0)
    col = lax.broadcasted_iota(jnp.int32, near_bias.shape[1:], 1)
    diff = (row % tile - col % tile) * 16 + row // tile - (col % near_rows) // tile
    diff = diff + jnp.where(col < near_rows, near_rows, 0)
    near_bias[0] = bias_of(diff, PATTERNS[0][0], col >= near_rows)
    near_bias[1] = bias_of(diff, PATTERNS[0][0], col >= 0)
    row = lax.broadcasted_iota(jnp.int32, mid_bias.shape[1:], 0)
    col = lax.broadcasted_iota(jnp.int32, mid_bias.shape[1:], 1)
    diff = (row % per_class - col % per_class) * 16
    diff = diff + 4 * (row // per_class - (col % mid_rows) // per_class)
    diff = diff + jnp.where(col < mid_rows, CLASSES * per_class, 0)
    mid_bias[0] = bias_of(diff, PATTERNS[1][0], col >= mid_rows)
    mid_bias[1] = bias_of(diff, PATTERNS[1][0], col >= 0)
    row = lax.broadcasted_iota(jnp.int32, far_bias.shape, 0)
    col = lax.broadcasted_iota(jnp.int32, far_bias.shape, 1)
    far_bias[...] = bias_of(row + REACH - col, REACH, col >= 0)

    lane = lax.broadcasted_iota(jnp.int32, (1, width), 1) // HEAD_DIM
    picks = [jnp.where(lane == h, HEAD_DIM ** -0.5, 0.0).astype(jnp.bfloat16) for h in range(heads)]

    def attend(queries, keys, values, bias):
        outs, tops, sums = [], [], []
        for h in range(heads):
            scores = lax.dot_general(
                queries * picks[h], keys, (((1,), (1,)), ((), ())), preferred_element_type=jnp.float32
            ) + bias
            top = jnp.max(scores, axis=1, keepdims=True)
            raised = jnp.exp(scores - top)
            total = jnp.sum(raised, axis=1, keepdims=True)
            outs.append(jnp.dot(raised.astype(jnp.bfloat16), values, preferred_element_type=jnp.float32))
            tops.append(jnp.broadcast_to(top, outs[-1].shape))
            sums.append(jnp.broadcast_to(total, outs[-1].shape))

        def join(parts):
            whole = parts[0]
            for h in range(1, heads):
                whole = jnp.where(lane == h, parts[h], whole)
            return whole

        return join(outs), join(tops), join(sums)

    def merge_rows(ref, *index):
        block = ref[index]
        return block.reshape(-1, width)

    @pl.loop(0, chunks)
    def near_and_mid(z):
        before = jnp.maximum(z - 1, 0)
        first = jnp.minimum(z, 1)
        for u in range(per_class // tile):
            rows = slice(u * tile, (u + 1) * tile)
            back, back_rows, kind = (before, slice(per_class - tile, per_class), first)
            if u > 0:
                back, back_rows, kind = (z, slice((u - 1) * tile, u * tile), 1)
            queries = q_ref[z, :, rows, :].reshape(near_rows, width)
            keys, values = (
                jnp.concatenate(
                    [
                        ref[back, :, back_rows, :].reshape(near_rows, width),
                        ref[z, :, rows, :].reshape(near_rows, width),
                    ],
                    axis=0,
                )
                for ref in (k_ref, v_ref)
            )
            for ref, part in zip((out_sc, top_sc, sum_sc), attend(queries, keys, values, near_bias[kind])):
                ref[0, z, :, rows, :] = part.reshape(CLASSES, tile, width)
        for r in range(4):
            classes = range(r, CLASSES, 4)
            queries = jnp.concatenate([q_ref[z, c] for c in classes], axis=0)
            keys, values = (
                jnp.concatenate([ref[y, c] for y in (before, z) for c in classes], axis=0)
                for ref in (k_ref, v_ref)
            )
            for ref, part in zip((out_sc, top_sc, sum_sc), attend(queries, keys, values, mid_bias[first])):
                for m, c in enumerate(classes):
                    ref[1, z, c] = part[m * per_class : (m + 1) * per_class]

    @pl.loop(0, CLASSES // 4)
    def far(quad):
        for inner in range(4):
            c = quad * 4 + inner
            for n in range(far_tiles):
                here = slice(n * span, (n + 1) * span)
                reach = slice(max(n - 1, 0) * span, (n + 1) * span)
                queries = q_ref[here, c].reshape(REACH, width)
                keys, values = (ref[reach, c].reshape(-1, width) for ref in (k_ref, v_ref))
                bias = far_bias[...] if n > 0 else far_bias[:, REACH:]
                for ref, part in zip((out_sc, top_sc, sum_sc), attend(queries, keys, values, bias)):
                    ref[2, here, c] = part.reshape(span, per_class, width)

    @pl.loop(0, chunks)
    def mix(z):
        tops = [top_sc[p, z] for p in range(3)]
        highest = jnp.maximum(jnp.maximum(tops[0], tops[1]), tops[2])
        lifts = [jnp.exp(top - highest) for top in tops]
        total = sum(lift * sum_sc[p, z] for p, lift in enumerate(lifts))
        result = sum(lift * out_sc[p, z] for p, lift in enumerate(lifts))
        o_ref[z] = (result / total).astype(o_ref.dtype)


def attend_all(moved, width):
    chunks, batches, _, per_class, triple = moved.shape
    channels = triple // 3
    pairs = channels // width
    if width % 128 == 0:
        operands = (moved, moved, moved)
        starts = (0, pairs, 2 * pairs)
    else:
        operands = tuple(moved[..., i * channels : (i + 1) * channels] for i in range(3))
        starts = (0, 0, 0)
    block = (chunks, None, CLASSES, per_class, width)
    tokens = chunks * CLASSES * per_class
    return pl.pallas_call(
        attend_kernel,
        grid=(batches, pairs),
        in_specs=[
            pl.BlockSpec(block, functools.partial(lambda s, b, i: (0, b, 0, 0, s + i), start)) for start in starts
        ],
        out_specs=pl.BlockSpec(block, lambda b, i: (0, b, 0, 0, i)),
        out_shape=jax.ShapeDtypeStruct((chunks, batches, CLASSES, per_class, channels), jnp.bfloat16),
        scratch_shapes=[pltpu.VMEM((3, chunks, CLASSES, per_class, width), jnp.float32) for _ in range(3)]
        + [
            pltpu.VMEM((2, 256, 512), jnp.float32),
            pltpu.VMEM((2, 4 * per_class, 8 * per_class), jnp.float32),
            pltpu.VMEM((REACH, 2 * REACH), jnp.float32),
        ],
        cost_estimate=pl.CostEstimate(
            flops=tokens * batches * channels * 4 * 900,
            bytes_accessed=tokens * batches * channels * 8,
            transcendentals=tokens * batches * channels // HEAD_DIM * 900,
        ),
    )(*operands)


def project_kernel(tokens_ref, weight_ref, *refs):
    *out_refs, product = refs
    step = pl.program_id(0)
    positions, batch_size, features = tokens_ref.shape
    rows = positions * batch_size
    flat = tokens_ref[...].reshape(rows, features)
    at = pl.ds(pl.multiple_of(step * rows, rows), rows)
    total = jnp.dot(flat, weight_ref[...], preferred_element_type=jnp.float32)
    for part in range(product.shape[0]):
        product[part, at, :] = total[:, part * LANES : (part + 1) * LANES]

    @pl.when(step == pl.num_programs(0) - 1)
    def leave():
        parts = product.shape[0] // len(out_refs)
        per_class = out_refs[0].shape[2]

        @pl.loop(0, CLASSES)
        def of_class(c):
            for part in range(product.shape[0]):
                out_ref, first = out_refs[part // parts], part % parts * LANES
                for b in range(batch_size):
                    picked = pl.ds(c * batch_size + b, per_class, stride=CLASSES * batch_size)
                    out_ref[b, c, :, first : first + LANES] = product[part, picked, :].astype(out_ref.dtype)


def project(tokens, weight, groups):
    seq_rows, batch_size, features = tokens.shape
    columns = weight.shape[1]
    per_class = seq_rows // CLASSES
    block = min(64, seq_rows)
    shape = (batch_size, CLASSES, per_class, columns // groups)
    return pl.pallas_call(
        project_kernel,
        grid=(seq_rows // block,),
        in_specs=[
            pl.BlockSpec((block, batch_size, features), lambda i: (i, 0, 0)),
            pl.BlockSpec(weight.shape, lambda i: (0, 0)),
        ],
        out_specs=[pl.BlockSpec(shape, lambda i: (0, 0, 0, 0))] * groups,
        out_shape=[jax.ShapeDtypeStruct(shape, jnp.bfloat16)] * groups,
        scratch_shapes=[pltpu.VMEM((columns // LANES, seq_rows * batch_size, LANES), jnp.float32)],
        compiler_params=pltpu.CompilerParams(dimension_semantics=("arbitrary",)),
        cost_estimate=pl.CostEstimate(
            flops=2 * seq_rows * batch_size * features * columns,
            bytes_accessed=2 * (tokens.size + weight.size + seq_rows * batch_size * columns),
            transcendentals=0,
        ),
    )(tokens, weight)


def body(tokens, query_weight, key_weight, value_weight, mix_gain, out_weight):
    seq_rows, batch_size, features = tokens.shape
    channels = query_weight.shape[1]
    sp_count = lax.axis_size("sp")
    tp_count = lax.axis_size("tp")
    tp_place = lax.axis_index("tp")
    per_class = seq_rows // CLASSES
    head_split = min(max(1, sp_count // batch_size), channels // HEAD_DIM)
    copies = max(1, sp_count // (batch_size * head_split))
    batches = max(1, batch_size // sp_count)
    groups = GROUPS if head_split == 1 else 1

    own = (out_weight.astype(jnp.float32) * mix_gain[:, None]).astype(jnp.bfloat16)
    gathered, sources, step = own, [0], tp_count // 2
    while step:
        route = [(i, i ^ step) for i in range(tp_count)]
        gathered = jnp.concatenate([gathered, lax.ppermute(gathered, "tp", route)], axis=0)
        sources += [s ^ step for s in sources]
        step //= 2

    cut = channels // groups // head_split
    width = min(cut, 2 * HEAD_DIM)
    columns = []
    for g in range(groups * head_split):
        columns += [w[:, g * cut : (g + 1) * cut] for w in (query_weight, key_weight, value_weight)]
    products = project(tokens, jnp.concatenate(columns, axis=1), groups)
    results = []
    for g, product in enumerate(products):
        if head_split > 1:
            product = product.reshape(batch_size, seq_rows, head_split, 3 * cut).transpose(0, 2, 1, 3)
        product = product.reshape(sp_count // copies, batches * seq_rows, 3 * cut)
        if copies > 1:
            product = jnp.repeat(product, copies, axis=0)
        moved = lax.all_to_all(product, "sp", split_axis=0, concat_axis=0, tiled=True)
        if g == 0:
            moved, gathered = lax.optimization_barrier((moved, gathered))
        moved = moved.reshape(sp_count, batches, CLASSES, per_class, 3 * cut)
        results.append(attend_all(moved, width))

    part = per_class // tp_count
    backs = []
    for result in results:
        back = result.reshape(sp_count, batches, CLASSES, tp_count, part, cut).transpose(0, 3, 1, 2, 4, 5)
        back = back.reshape(sp_count * tp_count, batches * CLASSES * part, cut)
        back = lax.all_to_all(back, ("sp", "tp"), split_axis=0, concat_axis=0, tiled=True)
        back = back.reshape(batch_size // batches, head_split, copies, tp_count, batches, CLASSES, part, cut)[:, :, 0]
        backs.append(back)
    combined = jnp.stack(backs, axis=0).transpose(3, 6, 5, 1, 4, 0, 2, 7)
    rows = part * CLASSES * batch_size
    combined = combined.reshape(tp_count, rows, channels)
    turned = jnp.concatenate(
        [lax.dynamic_index_in_dim(combined, tp_place ^ s, axis=0, keepdims=False) for s in sources], axis=1
    )
    wide = turned.astype(jnp.float32)
    row_scale = lax.rsqrt(jnp.mean(wide * wide, axis=-1, keepdims=True) + EPSILON)
    mixed = jnp.dot(turned, gathered, preferred_element_type=jnp.float32) * row_scale
    return mixed.astype(jnp.bfloat16).reshape(part * CLASSES, batch_size, out_weight.shape[1])


def solution(mesh):
    in_specs = (
        P("sp", "grp", None),
        P(None, "tp"),
        P(None, "tp"),
        P(None, "tp"),
        P("tp"),
        P("tp", None),
    )
    out_specs = P(("sp", "tp"), "grp", None)
    return jax.shard_map(body, mesh=mesh, in_specs=in_specs, out_specs=out_specs, check_vma=False)
```

```python
import functools

import jax
import jax.numpy as jnp
from jax import lax
from jax.experimental import pallas as pl
from jax.experimental.pallas import tpu as pltpu
from jax.sharding import PartitionSpec as P

HEAD_DIM = 64
PATTERNS = ((128, 1), (512, 4), (2048, 16))
REACH = 128
CLASSES = 16
LANES = 128
EPSILON = 1e-06
NEGATIVE = -1e30
GROUPS = 2


def attend_kernel(q_ref, k_ref, v_ref, o_ref, out_sc, top_sc, sum_sc, near_bias, mid_bias, far_bias):
    chunks, _, per_class, width = q_ref.shape
    heads = width // HEAD_DIM
    tile = 16
    near_rows = CLASSES * tile
    mid_rows = 4 * per_class
    span = REACH // per_class
    far_tiles = chunks // span

    def bias_of(diff, window, live):
        return jnp.where((diff >= 0) & (diff <= window) & live, 0.0, NEGATIVE).astype(jnp.float32)

    row = lax.broadcasted_iota(jnp.int32, near_bias.shape[1:], 0)
    col = lax.broadcasted_iota(jnp.int32, near_bias.shape[1:], 1)
    diff = (row % tile - col % tile) * 16 + row // tile - (col % near_rows) // tile
    diff = diff + jnp.where(col < near_rows, near_rows, 0)
    near_bias[0] = bias_of(diff, PATTERNS[0][0], col >= near_rows)
    near_bias[1] = bias_of(diff, PATTERNS[0][0], col >= 0)
    row = lax.broadcasted_iota(jnp.int32, mid_bias.shape[1:], 0)
    col = lax.broadcasted_iota(jnp.int32, mid_bias.shape[1:], 1)
    diff = (row % per_class - col % per_class) * 16
    diff = diff + 4 * (row // per_class - (col % mid_rows) // per_class)
    diff = diff + jnp.where(col < mid_rows, CLASSES * per_class, 0)
    mid_bias[0] = bias_of(diff, PATTERNS[1][0], col >= mid_rows)
    mid_bias[1] = bias_of(diff, PATTERNS[1][0], col >= 0)
    row = lax.broadcasted_iota(jnp.int32, far_bias.shape, 0)
    col = lax.broadcasted_iota(jnp.int32, far_bias.shape, 1)
    far_bias[...] = bias_of(row + REACH - col, REACH, col >= 0)

    lane = lax.broadcasted_iota(jnp.int32, (1, width), 1) // HEAD_DIM
    picks = [jnp.where(lane == h, HEAD_DIM ** -0.5, 0.0).astype(jnp.bfloat16) for h in range(heads)]

    def attend(queries, keys, values, bias):
        outs, tops, sums = [], [], []
        for h in range(heads):
            scores = lax.dot_general(
                queries * picks[h], keys, (((1,), (1,)), ((), ())), preferred_element_type=jnp.float32
            ) + bias
            top = jnp.max(scores, axis=1, keepdims=True)
            raised = jnp.exp(scores - top)
            total = jnp.sum(raised, axis=1, keepdims=True)
            outs.append(jnp.dot(raised.astype(jnp.bfloat16), values, preferred_element_type=jnp.float32))
            tops.append(jnp.broadcast_to(top, outs[-1].shape))
            sums.append(jnp.broadcast_to(total, outs[-1].shape))

        def join(parts):
            whole = parts[0]
            for h in range(1, heads):
                whole = jnp.where(lane == h, parts[h], whole)
            return whole

        return join(outs), join(tops), join(sums)

    def merge_rows(ref, *index):
        block = ref[index]
        return block.reshape(-1, width)

    @pl.loop(0, chunks)
    def near_and_mid(z):
        before = jnp.maximum(z - 1, 0)
        first = jnp.minimum(z, 1)
        for u in range(per_class // tile):
            rows = slice(u * tile, (u + 1) * tile)
            back, back_rows, kind = (before, slice(per_class - tile, per_class), first)
            if u > 0:
                back, back_rows, kind = (z, slice((u - 1) * tile, u * tile), 1)
            queries = q_ref[z, :, rows, :].reshape(near_rows, width)
            keys, values = (
                jnp.concatenate(
                    [
                        ref[back, :, back_rows, :].reshape(near_rows, width),
                        ref[z, :, rows, :].reshape(near_rows, width),
                    ],
                    axis=0,
                )
                for ref in (k_ref, v_ref)
            )
            for ref, part in zip((out_sc, top_sc, sum_sc), attend(queries, keys, values, near_bias[kind])):
                ref[0, z, :, rows, :] = part.reshape(CLASSES, tile, width)
        for r in range(4):
            classes = range(r, CLASSES, 4)
            queries = jnp.concatenate([q_ref[z, c] for c in classes], axis=0)
            keys, values = (
                jnp.concatenate([ref[y, c] for y in (before, z) for c in classes], axis=0)
                for ref in (k_ref, v_ref)
            )
            for ref, part in zip((out_sc, top_sc, sum_sc), attend(queries, keys, values, mid_bias[first])):
                for m, c in enumerate(classes):
                    ref[1, z, c] = part[m * per_class : (m + 1) * per_class]

    @pl.loop(0, CLASSES // 4)
    def far(quad):
        for inner in range(4):
            c = quad * 4 + inner
            for n in range(far_tiles):
                here = slice(n * span, (n + 1) * span)
                reach = slice(max(n - 1, 0) * span, (n + 1) * span)
                queries = q_ref[here, c].reshape(REACH, width)
                keys, values = (ref[reach, c].reshape(-1, width) for ref in (k_ref, v_ref))
                bias = far_bias[...] if n > 0 else far_bias[:, REACH:]
                for ref, part in zip((out_sc, top_sc, sum_sc), attend(queries, keys, values, bias)):
                    ref[2, here, c] = part.reshape(span, per_class, width)

    @pl.loop(0, chunks)
    def mix(z):
        tops = [top_sc[p, z] for p in range(3)]
        highest = jnp.maximum(jnp.maximum(tops[0], tops[1]), tops[2])
        lifts = [jnp.exp(top - highest) for top in tops]
        total = sum(lift * sum_sc[p, z] for p, lift in enumerate(lifts))
        result = sum(lift * out_sc[p, z] for p, lift in enumerate(lifts))
        o_ref[z] = (result / total).astype(o_ref.dtype)


def attend_all(moved, width):
    chunks, batches, _, per_class, triple = moved.shape
    channels = triple // 3
    pairs = channels // width
    if width % 128 == 0:
        operands = (moved, moved, moved)
        starts = (0, pairs, 2 * pairs)
    else:
        operands = tuple(moved[..., i * channels : (i + 1) * channels] for i in range(3))
        starts = (0, 0, 0)
    block = (chunks, None, CLASSES, per_class, width)
    tokens = chunks * CLASSES * per_class
    return pl.pallas_call(
        attend_kernel,
        grid=(batches, pairs),
        in_specs=[
            pl.BlockSpec(block, functools.partial(lambda s, b, i: (0, b, 0, 0, s + i), start)) for start in starts
        ],
        out_specs=pl.BlockSpec(block, lambda b, i: (0, b, 0, 0, i)),
        out_shape=jax.ShapeDtypeStruct((chunks, batches, CLASSES, per_class, channels), jnp.bfloat16),
        scratch_shapes=[pltpu.VMEM((3, chunks, CLASSES, per_class, width), jnp.float32) for _ in range(3)]
        + [
            pltpu.VMEM((2, 256, 512), jnp.float32),
            pltpu.VMEM((2, 4 * per_class, 8 * per_class), jnp.float32),
            pltpu.VMEM((REACH, 2 * REACH), jnp.float32),
        ],
        cost_estimate=pl.CostEstimate(
            flops=tokens * batches * channels * 4 * 900,
            bytes_accessed=tokens * batches * channels * 8,
            transcendentals=tokens * batches * channels // HEAD_DIM * 900,
        ),
    )(*operands)


def project_kernel(weight_count, places, tokens_ref, *refs):
    weight_refs, out_ref, product = refs[:weight_count], refs[weight_count], refs[-1]
    step = pl.program_id(0)
    positions, batch_size, features = tokens_ref.shape
    rows = positions * batch_size
    flat = tokens_ref[...].reshape(rows, features)
    at = pl.ds(pl.multiple_of(step * rows, rows), rows)
    for weight_ref, parts in zip(weight_refs, places):
        total = jnp.dot(flat, weight_ref[...], preferred_element_type=jnp.float32)
        for i, part in enumerate(parts):
            product[part, at, :] = total[:, i * LANES : (i + 1) * LANES]

    @pl.when(step == pl.num_programs(0) - 1)
    def leave():
        per_class = out_ref.shape[2]

        @pl.loop(0, CLASSES)
        def of_class(c):
            for part in range(product.shape[0]):
                for b in range(batch_size):
                    picked = pl.ds(c * batch_size + b, per_class, stride=CLASSES * batch_size)
                    out_ref[b, c, :, part * LANES : (part + 1) * LANES] = product[part, picked, :].astype(out_ref.dtype)


def project(tokens, weights, group, cut):
    seq_rows, batch_size, features = tokens.shape
    columns = cut * len(weights)
    per_class = seq_rows // CLASSES
    block = min(64, seq_rows)
    shape = (batch_size, CLASSES, per_class, columns)
    each = cut // LANES
    places = [range(w * each, (w + 1) * each) for w in range(len(weights))]
    return pl.pallas_call(
        functools.partial(project_kernel, len(weights), places),
        grid=(seq_rows // block,),
        in_specs=[pl.BlockSpec((block, batch_size, features), lambda i: (i, 0, 0))]
        + [pl.BlockSpec((features, cut), lambda i: (0, group))] * len(weights),
        out_specs=pl.BlockSpec(shape, lambda i: (0, 0, 0, 0)),
        out_shape=jax.ShapeDtypeStruct(shape, jnp.bfloat16),
        scratch_shapes=[pltpu.VMEM((columns // LANES, seq_rows * batch_size, LANES), jnp.float32)],
        compiler_params=pltpu.CompilerParams(dimension_semantics=("arbitrary",)),
        cost_estimate=pl.CostEstimate(
            flops=2 * seq_rows * batch_size * features * columns,
            bytes_accessed=2 * (tokens.size + features * columns + seq_rows * batch_size * columns),
            transcendentals=0,
        ),
    )(tokens, *weights)


def body(tokens, query_weight, key_weight, value_weight, mix_gain, out_weight):
    seq_rows, batch_size, features = tokens.shape
    channels = query_weight.shape[1]
    sp_count = lax.axis_size("sp")
    tp_count = lax.axis_size("tp")
    tp_place = lax.axis_index("tp")
    per_class = seq_rows // CLASSES
    head_split = min(max(1, sp_count // batch_size), channels // HEAD_DIM)
    copies = max(1, sp_count // (batch_size * head_split))
    batches = max(1, batch_size // sp_count)
    groups = GROUPS if head_split == 1 else 1

    own = (out_weight.astype(jnp.float32) * mix_gain[:, None]).astype(jnp.bfloat16)
    gathered, sources, step = own, [0], tp_count // 2
    while step:
        route = [(i, i ^ step) for i in range(tp_count)]
        gathered = jnp.concatenate([gathered, lax.ppermute(gathered, "tp", route)], axis=0)
        sources += [s ^ step for s in sources]
        step //= 2

    cut = channels // groups // head_split
    width = min(cut, 2 * HEAD_DIM)
    weights = (query_weight, key_weight, value_weight)
    results = []
    for g in range(groups):
        if cut % LANES == 0 and head_split == 1:
            product = project(tokens, weights, g, cut)
        else:
            spans = [slice(i * cut, (i + 1) * cut) for i in range(g * head_split, (g + 1) * head_split)]
            whole = jnp.concatenate([w[:, span] for span in spans for w in weights], axis=1)
            product = project(tokens, (whole,), 0, whole.shape[1])
        if head_split > 1:
            product = product.reshape(batch_size, seq_rows, head_split, 3 * cut).transpose(0, 2, 1, 3)
        product = product.reshape(sp_count // copies, batches * seq_rows, 3 * cut)
        if copies > 1:
            product = jnp.repeat(product, copies, axis=0)
        moved = lax.all_to_all(product, "sp", split_axis=0, concat_axis=0, tiled=True)
        if g == 0:
            moved, gathered = lax.optimization_barrier((moved, gathered))
        moved = moved.reshape(sp_count, batches, CLASSES, per_class, 3 * cut)
        results.append(attend_all(moved, width))

    part = per_class // tp_count
    backs = []
    for result in results:
        back = result.reshape(sp_count, batches, CLASSES, tp_count, part, cut).transpose(0, 3, 1, 2, 4, 5)
        back = back.reshape(sp_count * tp_count, batches * CLASSES * part, cut)
        back = lax.all_to_all(back, ("sp", "tp"), split_axis=0, concat_axis=0, tiled=True)
        back = back.reshape(batch_size // batches, head_split, copies, tp_count, batches, CLASSES, part, cut)[:, :, 0]
        backs.append(back)
    combined = jnp.stack(backs, axis=0).transpose(3, 6, 5, 1, 4, 0, 2, 7)
    rows = part * CLASSES * batch_size
    combined = combined.reshape(tp_count, rows, channels)
    turned = jnp.concatenate(
        [lax.dynamic_index_in_dim(combined, tp_place ^ s, axis=0, keepdims=False) for s in sources], axis=1
    )
    wide = turned.astype(jnp.float32)
    row_scale = lax.rsqrt(jnp.mean(wide * wide, axis=-1, keepdims=True) + EPSILON)
    mixed = jnp.dot(turned, gathered, preferred_element_type=jnp.float32) * row_scale
    return mixed.astype(jnp.bfloat16).reshape(part * CLASSES, batch_size, out_weight.shape[1])


def solution(mesh):
    in_specs = (
        P("sp", "grp", None),
        P(None, "tp"),
        P(None, "tp"),
        P(None, "tp"),
        P("tp"),
        P("tp", None),
    )
    out_specs = P(("sp", "tp"), "grp", None)
    return jax.shard_map(body, mesh=mesh, in_specs=in_specs, out_specs=out_specs, check_vma=False)
```
